32 devices in a mesh: sp: 16 (over z, y, x), tp: 2 (over core).
Axes of the slice: x: 2, y: 2, z: 4, core: 2. Of those that a mesh axis runs over, the one named last changes fastest.
Arguments:
- receptance: bfloat16 [3072, 1024], P('sp', 'tp'), may hold values from -6 to 6
- head_keys: bfloat16 [3072, 1024], P('sp', 'tp'), may hold values from -6 to 6
- head_values: bfloat16 [3072, 1024], P('sp', 'tp'), may hold values from -6 to 6
- decay_preact: float32 [3072, 1024], P('sp', 'tp'), may hold values from -13.5 to -0.5
- learning_rate_preact: float32 [3072, 1024], P('sp', 'tp'), may hold values from -10.5 to 2.5
- output_gate_preact: bfloat16 [3072, 1024], P('sp', 'tp'), may hold values from -8 to 8
- self_token_weight: float32 [16, 64], P('tp'), may hold values from -0.6 to 0.6
- head_norm_gain: float32 [1024], P('tp'), may hold values from 0.1 to 1.9
- output_weight: bfloat16 [1024, 2048], P('tp'), may hold values from -0.1875 to 0.1875
- residual: bfloat16 [3072, 2048], P('sp'), may hold values from -6 to 6
- premixer_norm_gain: float32 [2048], replicated, may hold values from 0.1 to 1.9
- mixer_gate_weight: bfloat16 [2048, 5120], P('sp', 'tp'), may hold values from -0.125 to 0.125
- mixer_up_weight: bfloat16 [2048, 5120], P('sp', 'tp'), may hold values from -0.125 to 0.125
- mixer_down_weight: bfloat16 [5120, 2048], P('tp', 'sp'), may hold values from -0.078125 to 0.078125
Outputs:
- layer_out: bfloat16 [3072, 2048], P(('sp', 'tp'))
The draws below stay inside these ranges and needn't reach their ends.
All inputs are finite; a program needn't handle non-finite values.
Results may differ from the reference program's by a relative error of at most 0.015.
Values may be sent and summed in bfloat16 or wider, within the bound.
A program may use at most 128 MiB of HBM per device.

```python
import jax
import jax.numpy as jnp
from jax import lax

D = 2048
WIDTH = 1024
HEAD_SIZE = 64
RECURRENT_HEADS = 16
FF = 5120
TOK_DEV = 192
TOKENS = 3072
N_TP = 2


def head_speed(key):
    chosen = jax.random.permutation(jax.random.fold_in(key, 4711), WIDTH // HEAD_SIZE)
    fast_count = WIDTH // HEAD_SIZE // 2
    return chosen < fast_count


def draw_decay_preact(key, part):
    fast_heads = head_speed(key)
    head_total = WIDTH // HEAD_SIZE
    keys_all = jax.random.split(jax.random.fold_in(key, 17), 5)
    fast_base = jax.random.uniform(keys_all[0], (head_total,), jnp.float32, -3.5, -2.5)
    slow_base = jax.random.uniform(keys_all[1], (head_total,), jnp.float32, -11.5, -10.5)
    head_base = jnp.where(fast_heads, fast_base, slow_base)
    shards = TOKENS // TOK_DEV
    block_shift = jax.random.uniform(keys_all[2], (shards, head_total), jnp.float32, -1.0, 1.0)
    block_shift = jnp.repeat(block_shift, TOK_DEV, axis=0)
    jitter = jax.random.uniform(keys_all[3], (TOKENS, head_total, HEAD_SIZE), jnp.float32, -1.0, 1.0)
    return (head_base[None, :, None] + block_shift[:, :, None] + jitter).reshape(TOKENS, WIDTH)


def draw_learning_rate_preact(key, part):
    fast_heads = head_speed(key)
    head_total = WIDTH // HEAD_SIZE
    keys_all = jax.random.split(jax.random.fold_in(key, 29), 2)
    fast_part = jax.random.uniform(keys_all[0], (TOKENS, head_total, HEAD_SIZE), jnp.float32, -2.5, 2.5)
    slow_part = jax.random.uniform(keys_all[1], (TOKENS, head_total, HEAD_SIZE), jnp.float32, -10.5, -7.5)
    return jnp.where(fast_heads[None, :, None], fast_part, slow_part).reshape(TOKENS, WIDTH)


def block_scale(own_key, dims, cuts, smallest, high):
    factor_of, own = 1.0, jax.random.fold_in(own_key, 6)
    for axis_at, shards_of in cuts:
        draws = jnp.exp(jax.random.uniform(jax.random.fold_in(own, axis_at), (shards_of,), jnp.float32, smallest / len(cuts), high / len(cuts)))
        factor_of = factor_of * jnp.repeat(draws, dims[axis_at] // shards_of).reshape([-1 if axis == axis_at else 1 for axis in range(len(dims))])
    return factor_of


def centred(key, shape, scale, most, cuts=(), held_as=jnp.bfloat16):
    drawn = jax.random.normal(key, shape, jnp.float32) * scale
    if len(cuts) > 0:
        drawn = block_scale(key, shape, cuts, -0.22, 0.18) * drawn
    return jnp.clip(drawn, min=-most, max=most).astype(held_as)


def setup_inputs(seed: int = 0) -> dict:
    keys = jax.random.split(jax.random.key(seed), 15)
    return {
        "receptance": centred(keys[0], (TOKENS, WIDTH), 1.0, 6.0, ((0, 16), (1, 2))),
        "head_keys": centred(keys[1], (TOKENS, WIDTH), 1.0, 6.0, ((0, 16), (1, 2))),
        "head_values": centred(keys[2], (TOKENS, WIDTH), 1.0, 6.0, ((0, 16), (1, 2))),
        "decay_preact": draw_decay_preact(jax.random.fold_in(keys[14], 71), 0),
        "learning_rate_preact": draw_learning_rate_preact(jax.random.fold_in(keys[14], 71), 0),
        "output_gate_preact": centred(keys[5], (TOKENS, WIDTH), 1.5, 8.0, ((0, 16), (1, 2))),
        "self_token_weight": centred(keys[6], (RECURRENT_HEADS, HEAD_SIZE), 0.1, 0.6, ((0, 2),), jnp.float32),
        "head_norm_gain": jnp.clip(1.0 + 0.18 * jax.random.normal(keys[7], (WIDTH,), jnp.float32), 0.1, 1.9),
        "output_weight": centred(keys[8], (WIDTH, D), WIDTH ** -0.5, 0.1875, ((0, 2),)),
        "residual": centred(keys[9], (TOKENS, D), 1.0, 6.0, ((0, 16),)),
        "premixer_norm_gain": jnp.clip(1.0 + 0.18 * jax.random.normal(keys[10], (D,), jnp.float32), 0.1, 1.9),
        "mixer_gate_weight": centred(keys[11], (D, FF), D ** -0.5, 0.125, ((0, 16), (1, 2))),
        "mixer_up_weight": centred(keys[12], (D, FF), D ** -0.5, 0.125, ((0, 16), (1, 2))),
        "mixer_down_weight": centred(keys[13], (FF, D), FF ** -0.5, 0.078125, ((0, 2), (1, 16))),
    }


GROUP_EPS = 0.00064
NORM_EPS = 1e-06
EXACT = lax.Precision.HIGHEST

def final_output(layer_result, receptance_rows, keys_single, values_single, self_token_weight, head_norm_gain, output_gate_preact):
    centre = lax.optimization_barrier(jnp.mean(layer_result, axis=-1, keepdims=True))
    spread = lax.optimization_barrier(jnp.mean(jnp.square(layer_result - centre), axis=-1, keepdims=True))
    scaled_rows = (layer_result - centre) * lax.rsqrt(spread + GROUP_EPS)
    self_token_term = lax.optimization_barrier(jnp.sum(receptance_rows * keys_single * self_token_weight[None], axis=-1, keepdims=True)) * values_single
    sequence_length = layer_result.shape[0]
    heads_merged = scaled_rows.reshape(sequence_length, -1) * head_norm_gain[None] + self_token_term.reshape(sequence_length, -1)
    return (heads_merged * jax.nn.sigmoid(output_gate_preact.astype(jnp.float32))).astype(jnp.bfloat16)

def reference(receptance, head_keys, head_values, decay_preact, learning_rate_preact, output_gate_preact, self_token_weight, head_norm_gain, output_weight, residual, premixer_norm_gain, mixer_gate_weight, mixer_up_weight, mixer_down_weight):
    sequence_length = receptance.shape[0]
    head_count = WIDTH // HEAD_SIZE
    layout = (sequence_length, head_count, HEAD_SIZE)
    receptance_rows = receptance.astype(jnp.float32).reshape(layout)
    keys_single = head_keys.astype(jnp.float32).reshape(layout)
    values_single = head_values.astype(jnp.float32).reshape(layout)
    decay_rate = jnp.exp(-jnp.exp(-jax.nn.softplus(-decay_preact) - 0.5)).reshape(layout)
    learn_rate = jax.nn.sigmoid(learning_rate_preact).reshape(layout)
    unit_key = keys_single / jnp.maximum(jnp.linalg.norm(keys_single, axis=-1, keepdims=True), 1.0)
    remove_dir = -unit_key
    insert_dir = unit_key * learn_rate

    def advance(memory, inputs):
        decay_t, key_t, value_t, remove_t, insert_t, recept_t = inputs
        erased = jnp.einsum('hij,hj->hi', memory, remove_t, precision=EXACT)
        memory = memory * decay_t[:, None, :] + erased[:, :, None] * insert_t[:, None, :] + value_t[:, :, None] * key_t[:, None, :]
        return (memory, jnp.einsum('hij,hj->hi', memory, recept_t, precision=EXACT))
    start_state = jnp.zeros((head_count, HEAD_SIZE, HEAD_SIZE), jnp.float32)
    _, recurrence_output = lax.scan(advance, start_state, (decay_rate, keys_single, values_single, remove_dir, insert_dir, receptance_rows))
    mixer_output = final_output(recurrence_output, receptance_rows, keys_single, values_single, self_token_weight, head_norm_gain, output_gate_preact)
    group = WIDTH // N_TP

    def add_group(total, which):
        begin = (which * group).astype(jnp.int32)
        columns = lax.dynamic_slice_in_dim(mixer_output, begin, group, 1)
        rows_part = lax.dynamic_slice_in_dim(output_weight, begin, group, 0)
        product = jnp.dot(columns.astype(jnp.float32), rows_part.astype(jnp.float32), preferred_element_type=jnp.float32)
        return (total + lax.optimization_barrier(product.astype(jnp.bfloat16)).astype(jnp.float32), None)
    mix_sum, _ = lax.scan(add_group, jnp.zeros((sequence_length, D), jnp.float32), jnp.arange(N_TP, dtype=jnp.int32))
    mix = lax.optimization_barrier(mix_sum.astype(jnp.bfloat16)).astype(jnp.float32)
    after_mix = (residual.astype(jnp.float32) + mix).astype(jnp.bfloat16)
    widened = after_mix.astype(jnp.float32)
    normed = (widened * lax.rsqrt(lax.optimization_barrier(jnp.mean(widened * widened, axis=-1, keepdims=True)) + NORM_EPS) * premixer_norm_gain[None]).astype(jnp.bfloat16)
    hidden_group = FF // N_TP

    def add_hidden(total, which):
        begin = (which * hidden_group).astype(jnp.int32)
        gate_sum = jnp.dot(normed.astype(jnp.float32), lax.dynamic_slice_in_dim(mixer_gate_weight, begin, hidden_group, 1).astype(jnp.float32), preferred_element_type=jnp.float32)
        up_sum = jnp.dot(normed.astype(jnp.float32), lax.dynamic_slice_in_dim(mixer_up_weight, begin, hidden_group, 1).astype(jnp.float32), preferred_element_type=jnp.float32)
        hidden = (jax.nn.silu(gate_sum) * up_sum).astype(jnp.bfloat16)
        product = jnp.dot(hidden.astype(jnp.float32), lax.dynamic_slice_in_dim(mixer_down_weight, begin, hidden_group, 0).astype(jnp.float32), preferred_element_type=jnp.float32)
        return (total + lax.optimization_barrier(product.astype(jnp.bfloat16)).astype(jnp.float32), None)
    down_sum, _ = lax.scan(add_hidden, jnp.zeros((sequence_length, D), jnp.float32), jnp.arange(N_TP, dtype=jnp.int32))
    return (after_mix.astype(jnp.float32) + down_sum).astype(jnp.bfloat16)
```

```python
import functools

import jax
import jax.numpy as jnp
from jax import lax
from jax.experimental import pallas as pl
from jax.experimental.pallas import tpu as pltpu
from jax.sharding import PartitionSpec as P

HEAD = 64
LANES = 2 * HEAD
GROUP_EPS = 0.00064
NORM_EPS = 1e-06
NN = (((1,), (0,)), ((), ()))
NT = (((1,), (1,)), ((), ()))
TN = (((0,), (0,)), ((), ()))
INNER = 4


def split(x):
    high = x.astype(jnp.bfloat16)
    return high, (x - high.astype(jnp.float32)).astype(jnp.bfloat16)


def dot1(a, b, dims=NN):
    return lax.dot_general(
        a.astype(jnp.bfloat16), b.astype(jnp.bfloat16), dims, preferred_element_type=jnp.float32
    )


def dot3(a, b, dims=NN):
    ah, al = a if isinstance(a, tuple) else split(a)
    bh, bl = b if isinstance(b, tuple) else split(b)
    d = functools.partial(
        lax.dot_general, dimension_numbers=dims, preferred_element_type=jnp.float32
    )
    return d(ah, bh) + (d(ah, bl) + d(al, bh))


def per_head_sum(x, first):
    s0 = jnp.sum(jnp.where(first, x, 0.0), axis=-1, keepdims=True)
    s1 = jnp.sum(jnp.where(first, 0.0, x), axis=-1, keepdims=True)
    return jnp.where(first, s0, s1)


def block_diag_mask():
    row = lax.broadcasted_iota(jnp.int32, (LANES, LANES), 0)
    col = lax.broadcasted_iota(jnp.int32, (LANES, LANES), 1)
    return row // HEAD == col // HEAD, row == col


def fold(full):
    mask, _ = block_diag_mask()
    kept = jnp.where(mask, full, 0.0)
    return kept[:HEAD] + kept[HEAD:]


def unfold(packed):
    mask, _ = block_diag_mask()
    return jnp.where(mask, jnp.concatenate([packed, packed], axis=0), 0.0)


def local_kernel(r_ref, k_ref, v_ref, dw_ref, lw_ref, q_ref, y_ref, ps_ref):
    steps = r_ref.shape[0]
    f32 = jnp.float32
    first = lax.broadcasted_iota(jnp.int32, (steps, LANES), 1) < HEAD
    row = lax.broadcasted_iota(jnp.int32, (steps, steps), 0)
    col = lax.broadcasted_iota(jnp.int32, (steps, steps), 1)
    r, k, v = (x[...].astype(f32) for x in (r_ref, k_ref, v_ref))
    log_decay = jax.nn.sigmoid(dw_ref[...]) * (-0.6065306597126334)
    ones = (row >= col).astype(jnp.bfloat16)
    h0 = log_decay.astype(jnp.bfloat16)
    rest = log_decay - h0.astype(f32)
    h1 = rest.astype(jnp.bfloat16)
    h2 = (rest - h1.astype(f32)).astype(jnp.bfloat16)
    total = dot1(ones, h0) + (dot1(ones, h1) + dot1(ones, h2))
    last = total[steps - 1 :, :]
    unit = k / jnp.maximum(jnp.sqrt(per_head_sum(k * k, first)), 1.0)
    insert = unit * jax.nn.sigmoid(lw_ref[...])
    undo = jnp.exp(-total)
    remaining = jnp.exp(last - total)
    a_bar = -unit * jnp.exp(total - log_decay)
    r_bar = r * jnp.exp(total)
    b_hat = insert * undo
    k_hat = k * undo
    right = split(jnp.concatenate([b_hat, k_hat], axis=0))
    left = jnp.concatenate([a_bar, r_bar], axis=0)
    first2 = jnp.concatenate([first, first], axis=0)
    grams = [
        dot3(jnp.where(first2 if h == 0 else ~first2, left, 0.0), right, NT) for h in (0, 1)
    ]
    strict, incl = row > col, row >= col
    ab = [jnp.where(strict, g[:steps, :steps], 0.0) for g in grams]
    ak = [jnp.where(strict, g[:steps, steps:], 0.0) for g in grams]
    rb = [jnp.where(incl, g[steps:, :steps], 0.0) for g in grams]
    rk = [jnp.where(incl, g[steps:, steps:], 0.0) for g in grams]
    vb = v_ref[...]

    def times_v(m):
        mh, ml = split(m)
        return dot1(mh, vb) + dot1(ml, vb)

    seeds = [jnp.concatenate([a_bar, times_v(m)], axis=1) for m in ak]
    ab16 = [m.astype(jnp.bfloat16) for m in ab]
    eye = (row == col).astype(f32)
    size = 1
    inv = None
    while size < steps:
        joined = (
            (row // (2 * size) == col // (2 * size))
            & ((row // size) % 2 == 1)
            & ((col // size) % 2 == 0)
        )
        parts = [jnp.where(joined, m, jnp.zeros_like(m)) for m in ab16]
        if inv is None:
            inv = [eye + p.astype(f32) for p in parts]
        else:
            t16 = [t.astype(jnp.bfloat16) for t in inv]
            mid = [dot1(t, p) for t, p in zip(t16, parts)]
            inv = [t + dot1(m, tt) for t, m, tt in zip(inv, mid, t16)]
        size *= 2
    inv16 = [t.astype(jnp.bfloat16) for t in inv]
    absp = [split(m) for m in ab]
    sol = [dot1(t, s) for t, s in zip(inv16, seeds)]
    for _ in range(2):
        res = [s - x + dot3(m, x) for s, x, m in zip(seeds, sol, absp)]
        sol = [x + dot1(t, e) for x, t, e in zip(sol, inv16, res)]
    outs = [dot3(m, x) for m, x in zip(rb, sol)]
    own = [times_v(m) for m in rk]
    q_ref[...] = r_bar + jnp.where(first, outs[0][:, :LANES], outs[1][:, :LANES])
    y_ref[...] = jnp.where(first, outs[0][:, LANES:] + own[0], outs[1][:, LANES:] + own[1])
    w = jnp.where(first, sol[0][:, :LANES], sol[1][:, :LANES])
    u = jnp.where(first, sol[0][:, LANES:], sol[1][:, LANES:])
    b_end = split(insert * remaining)
    _, diag = block_diag_mask()
    prod = dot3(w, b_end, TN) + jnp.where(diag, jnp.exp(last), 0.0)
    kh, kl = split(k * remaining)
    state = dot3(u, b_end, TN) + dot1(vb, kh, TN) + dot1(vb, kl, TN)
    ps_ref[0, 0] = fold(prod)
    ps_ref[0, 1] = fold(state)


def join_kernel(i_ref, ps_ref, q_ref, y_ref, r_ref, k_ref, v_ref, g_ref, tw_ref, hg_ref, w_ref, o_ref):
    steps = q_ref.shape[0]
    pairs = q_ref.shape[1] // LANES
    f32 = jnp.float32
    first = lax.broadcasted_iota(jnp.int32, (steps, LANES), 1) < HEAD

    def turn(j, states):
        return tuple(
            dot3(s, unfold(ps_ref[j, p, 0])) + unfold(ps_ref[j, p, 1])
            for p, s in enumerate(states)
        )

    zero = jnp.zeros((LANES, LANES), f32)
    states = lax.fori_loop(0, i_ref[0], turn, (zero,) * pairs)
    mixed = []
    for p in range(pairs):
        cut = slice(p * LANES, (p + 1) * LANES)
        y = dot3(q_ref[:, cut], states[p], NT) + y_ref[:, cut]
        y = y - per_head_sum(y, first) * (1.0 / HEAD)
        spread = per_head_sum(y * y, first) * (1.0 / HEAD)
        r, k, v = (x[:, cut].astype(f32) for x in (r_ref, k_ref, v_ref))
        own = per_head_sum(r * k * tw_ref[:, cut], first) * v
        out = y * lax.rsqrt(spread + GROUP_EPS) * hg_ref[:, cut] + own
        mixed.append((out * jax.nn.sigmoid(g_ref[:, cut].astype(f32))).astype(jnp.bfloat16))
    mixed = jnp.concatenate(mixed, axis=1)
    o_ref[...] = jnp.dot(mixed, w_ref[...], preferred_element_type=f32).astype(jnp.bfloat16)


def recurrence(r, k, v, dw, lw):
    steps, width = r.shape
    pairs = width // LANES
    cols = pl.BlockSpec((steps, LANES), lambda p: (0, p))
    return pl.pallas_call(
        local_kernel,
        grid=(pairs,),
        in_specs=[cols] * 5,
        out_specs=[cols, cols, pl.BlockSpec((1, 2, HEAD, LANES), lambda p: (p, 0, 0, 0))],
        out_shape=[
            jax.ShapeDtypeStruct((steps, width), jnp.float32),
            jax.ShapeDtypeStruct((steps, width), jnp.float32),
            jax.ShapeDtypeStruct((pairs, 2, HEAD, LANES), jnp.float32),
        ],
        cost_estimate=pl.CostEstimate(
            flops=20_000_000_000, bytes_accessed=4_000_000, transcendentals=1_000_000
        ),
        name="local_part",
    )(r, k, v, dw, lw)


def join(index, ps, q, y, r, k, v, gate, tw, hg, w):
    vmem = pl.BlockSpec(memory_space=pltpu.VMEM)
    return pl.pallas_call(
        join_kernel,
        in_specs=[pl.BlockSpec(memory_space=pltpu.SMEM)] + [vmem] * 10,
        out_specs=vmem,
        out_shape=jax.ShapeDtypeStruct((q.shape[0], w.shape[1]), jnp.bfloat16),
        cost_estimate=pl.CostEstimate(
            flops=10_000_000_000, bytes_accessed=8_000_000, transcendentals=100_000
        ),
        name="join_part",
    )(index, ps, q, y, r, k, v, gate, tw, hg, w)


def rms_scale(rows, gain):
    x = rows.astype(jnp.float32)
    factor = lax.rsqrt(jnp.mean(x * x, axis=-1, keepdims=True) + NORM_EPS)
    return (x * factor * gain[None]).astype(jnp.bfloat16)


def per_device(r, k, v, dw, lw, gate, tw, hg, w_out, residual, gain, w_gate, w_up, w_down):
    steps = r.shape[0]
    sp, tp = lax.axis_size("sp"), lax.axis_size("tp")
    inner = INNER if sp % INNER == 0 else 1
    near = [[g * inner + i for i in range(inner)] for g in range(sp // inner)]
    far = [[g * inner + i for g in range(sp // inner)] for i in range(inner)]
    hidden = w_gate.shape[1] // inner

    q, y, ps = recurrence(r, k, v, dw, lw)
    ps_all = lax.all_gather(ps, "sp")

    def by_columns(w):
        w = lax.all_to_all(
            w, "sp", split_axis=1, concat_axis=0, axis_index_groups=near, tiled=True
        )
        return lax.all_gather(w, "sp", axis_index_groups=far, axis=0, tiled=False)

    g_all, u_all = by_columns(w_gate), by_columns(w_up)
    g_all = g_all.reshape(-1, hidden)
    u_all = u_all.reshape(-1, hidden)
    d_part = lax.all_to_all(
        w_down, "sp", split_axis=0, concat_axis=1, axis_index_groups=near, tiled=True
    )
    d_all = lax.all_gather(d_part, "sp", axis_index_groups=far, axis=1, tiled=True)

    index = lax.axis_index("sp").astype(jnp.int32).reshape(1)
    part = join(
        index, ps_all, q, y, r, k, v, gate, tw.reshape(1, -1), hg.reshape(1, -1), w_out
    )
    own_rows = steps // tp
    start = lax.axis_index("tp") * own_rows
    mix = lax.all_to_all(part.reshape(tp, own_rows, -1), "tp", 0, 0)
    mix = jnp.sum(mix.astype(jnp.float32), axis=0).astype(jnp.bfloat16).astype(jnp.float32)
    mine = lax.dynamic_slice_in_dim(residual, start, own_rows, 0)
    after = (mine.astype(jnp.float32) + mix).astype(jnp.bfloat16)
    normed = lax.all_gather(rms_scale(after, gain), "tp", axis=0, tiled=True)
    normed = lax.all_gather(normed, "sp", axis_index_groups=near, axis=0, tiled=True)
    g = jnp.dot(normed, g_all, preferred_element_type=jnp.float32)
    u = jnp.dot(normed, u_all, preferred_element_type=jnp.float32)
    h = (jax.nn.silu(g) * u).astype(jnp.bfloat16)
    down = jnp.dot(h, d_all, preferred_element_type=jnp.float32).astype(jnp.bfloat16)
    down = down.reshape(inner, tp, own_rows, -1)
    down = lax.all_to_all(down, "sp", 0, 0, axis_index_groups=near)
    down = jnp.sum(down.astype(jnp.float32), axis=0).astype(jnp.bfloat16)
    down = lax.all_to_all(down, "tp", 0, 0)
    down = jnp.sum(down.astype(jnp.float32), axis=0)
    return (after.astype(jnp.float32) + down).astype(jnp.bfloat16)


def solution(mesh):
    split_both = P("sp", "tp")
    placed = (split_both,) * 6 + (
        P("tp", None),
        P("tp"),
        P("tp", None),
        P("sp", None),
        P(),
        split_both,
        split_both,
        P("tp", "sp"),
    )
    return jax.shard_map(
        per_device, mesh=mesh, in_specs=placed, out_specs=P(("sp", "tp"), None), check_vma=False
    )
```

```python
import functools

import jax
import jax.numpy as jnp
from jax import lax
from jax.experimental import pallas as pl
from jax.experimental.pallas import tpu as pltpu
from jax.sharding import PartitionSpec as P

HEAD = 64
LANES = 2 * HEAD
GROUP_EPS = 0.00064
NORM_EPS = 1e-06
NN = (((1,), (0,)), ((), ()))
NT = (((1,), (1,)), ((), ()))
TN = (((0,), (0,)), ((), ()))
INNER = 4
MESH = pl.DeviceIdType.MESH


def split(x):
    high = x.astype(jnp.bfloat16)
    return high, (x - high.astype(jnp.float32)).astype(jnp.bfloat16)


def dot1(a, b, dims=NN):
    return lax.dot_general(
        a.astype(jnp.bfloat16), b.astype(jnp.bfloat16), dims, preferred_element_type=jnp.float32
    )


def dot3(a, b, dims=NN):
    ah, al = a if isinstance(a, tuple) else split(a)
    bh, bl = b if isinstance(b, tuple) else split(b)
    d = functools.partial(
        lax.dot_general, dimension_numbers=dims, preferred_element_type=jnp.float32
    )
    return d(ah, bh) + (d(ah, bl) + d(al, bh))


def per_head_sum(x, first):
    s0 = jnp.sum(jnp.where(first, x, 0.0), axis=-1, keepdims=True)
    s1 = jnp.sum(jnp.where(first, 0.0, x), axis=-1, keepdims=True)
    return jnp.where(first, s0, s1)


def block_diag_mask():
    row = lax.broadcasted_iota(jnp.int32, (LANES, LANES), 0)
    col = lax.broadcasted_iota(jnp.int32, (LANES, LANES), 1)
    return row // HEAD == col // HEAD, row == col


def fold(full):
    mask, _ = block_diag_mask()
    kept = jnp.where(mask, full, 0.0)
    return kept[:HEAD] + kept[HEAD:]


def unfold(packed):
    mask, _ = block_diag_mask()
    return jnp.where(mask, jnp.concatenate([packed, packed], axis=0), 0.0)


def local_kernel(r_ref, k_ref, v_ref, dw_ref, lw_ref, q_ref, y_ref, ps_ref):
    steps = r_ref.shape[0]
    f32 = jnp.float32
    first = lax.broadcasted_iota(jnp.int32, (steps, LANES), 1) < HEAD
    row = lax.broadcasted_iota(jnp.int32, (steps, steps), 0)
    col = lax.broadcasted_iota(jnp.int32, (steps, steps), 1)
    r, k, v = (x[...].astype(f32) for x in (r_ref, k_ref, v_ref))
    log_decay = jax.nn.sigmoid(dw_ref[...]) * (-0.6065306597126334)
    ones = (row >= col).astype(jnp.bfloat16)
    h0 = log_decay.astype(jnp.bfloat16)
    rest = log_decay - h0.astype(f32)
    h1 = rest.astype(jnp.bfloat16)
    h2 = (rest - h1.astype(f32)).astype(jnp.bfloat16)
    total = dot1(ones, h0) + (dot1(ones, h1) + dot1(ones, h2))
    last = total[steps - 1 :, :]
    unit = k / jnp.maximum(jnp.sqrt(per_head_sum(k * k, first)), 1.0)
    insert = unit * jax.nn.sigmoid(lw_ref[...])
    undo = jnp.exp(-total)
    remaining = jnp.exp(last - total)
    a_bar = -unit * jnp.exp(total - log_decay)
    r_bar = r * jnp.exp(total)
    b_hat = insert * undo
    k_hat = k * undo
    right = split(jnp.concatenate([b_hat, k_hat], axis=0))
    left = jnp.concatenate([a_bar, r_bar], axis=0)
    first2 = jnp.concatenate([first, first], axis=0)
    grams = [
        dot3(jnp.where(first2 if h == 0 else ~first2, left, 0.0), right, NT) for h in (0, 1)
    ]
    strict, incl = row > col, row >= col
    ab = [jnp.where(strict, g[:steps, :steps], 0.0) for g in grams]
    ak = [jnp.where(strict, g[:steps, steps:], 0.0) for g in grams]
    rb = [jnp.where(incl, g[steps:, :steps], 0.0) for g in grams]
    rk = [jnp.where(incl, g[steps:, steps:], 0.0) for g in grams]
    vb = v_ref[...]

    def times_v(m):
        mh, ml = split(m)
        return dot1(mh, vb) + dot1(ml, vb)

    seeds = [jnp.concatenate([a_bar, times_v(m)], axis=1) for m in ak]
    ab16 = [m.astype(jnp.bfloat16) for m in ab]
    eye = (row == col).astype(f32)
    size = 1
    inv = None
    while size < steps:
        joined = (
            (row // (2 * size) == col // (2 * size))
            & ((row // size) % 2 == 1)
            & ((col // size) % 2 == 0)
        )
        parts = [jnp.where(joined, m, jnp.zeros_like(m)) for m in ab16]
        if inv is None:
            inv = [eye + p.astype(f32) for p in parts]
        else:
            t16 = [t.astype(jnp.bfloat16) for t in inv]
            mid = [dot1(t, p) for t, p in zip(t16, parts)]
            inv = [t + dot1(m, tt) for t, m, tt in zip(inv, mid, t16)]
        size *= 2
    inv16 = [t.astype(jnp.bfloat16) for t in inv]
    absp = [split(m) for m in ab]
    sol = [dot1(t, s) for t, s in zip(inv16, seeds)]
    for _ in range(2):
        res = [s - x + dot3(m, x) for s, x, m in zip(seeds, sol, absp)]
        sol = [x + dot1(t, e) for x, t, e in zip(sol, inv16, res)]
    outs = [dot3(m, x) for m, x in zip(rb, sol)]
    own = [times_v(m) for m in rk]
    q_ref[...] = r_bar + jnp.where(first, outs[0][:, :LANES], outs[1][:, :LANES])
    y_ref[...] = jnp.where(first, outs[0][:, LANES:] + own[0], outs[1][:, LANES:] + own[1])
    w = jnp.where(first, sol[0][:, :LANES], sol[1][:, :LANES])
    u = jnp.where(first, sol[0][:, LANES:], sol[1][:, LANES:])
    b_end = split(insert * remaining)
    _, diag = block_diag_mask()
    prod = dot3(w, b_end, TN) + jnp.where(diag, jnp.exp(last), 0.0)
    kh, kl = split(k * remaining)
    state = dot3(u, b_end, TN) + dot1(vb, kh, TN) + dot1(vb, kl, TN)
    ps_ref[0, 0] = fold(prod)
    ps_ref[0, 1] = fold(state)


def join_kernel(i_ref, ps_ref, q_ref, y_ref, r_ref, k_ref, v_ref, g_ref, tw_ref, hg_ref, w_ref, o_ref):
    steps = q_ref.shape[0]
    pairs = q_ref.shape[1] // LANES
    f32 = jnp.float32
    first = lax.broadcasted_iota(jnp.int32, (steps, LANES), 1) < HEAD

    def turn(j, states):
        return tuple(
            dot3(s, unfold(ps_ref[j, p, 0])) + unfold(ps_ref[j, p, 1])
            for p, s in enumerate(states)
        )

    zero = jnp.zeros((LANES, LANES), f32)
    states = lax.fori_loop(0, i_ref[0], turn, (zero,) * pairs)
    mixed = []
    for p in range(pairs):
        cut = slice(p * LANES, (p + 1) * LANES)
        y = dot3(q_ref[:, cut], states[p], NT) + y_ref[:, cut]
        y = y - per_head_sum(y, first) * (1.0 / HEAD)
        spread = per_head_sum(y * y, first) * (1.0 / HEAD)
        r, k, v = (x[:, cut].astype(f32) for x in (r_ref, k_ref, v_ref))
        own = per_head_sum(r * k * tw_ref[:, cut], first) * v
        out = y * lax.rsqrt(spread + GROUP_EPS) * hg_ref[:, cut] + own
        mixed.append((out * jax.nn.sigmoid(g_ref[:, cut].astype(f32))).astype(jnp.bfloat16))
    mixed = jnp.concatenate(mixed, axis=1)
    o_ref[...] = jnp.dot(mixed, w_ref[...], preferred_element_type=f32).astype(jnp.bfloat16)


def recurrence(r, k, v, dw, lw):
    steps, width = r.shape
    pairs = width // LANES
    cols = pl.BlockSpec((steps, LANES), lambda p: (0, p))
    return pl.pallas_call(
        local_kernel,
        grid=(pairs,),
        in_specs=[cols] * 5,
        out_specs=[cols, cols, pl.BlockSpec((1, 2, HEAD, LANES), lambda p: (p, 0, 0, 0))],
        out_shape=[
            jax.ShapeDtypeStruct((steps, width), jnp.float32),
            jax.ShapeDtypeStruct((steps, width), jnp.float32),
            jax.ShapeDtypeStruct((pairs, 2, HEAD, LANES), jnp.float32),
        ],
        cost_estimate=pl.CostEstimate(
            flops=20_000_000_000, bytes_accessed=4_000_000, transcendentals=1_000_000
        ),
        name="local_part",
    )(r, k, v, dw, lw)


def join(index, ps, q, y, r, k, v, gate, tw, hg, w):
    vmem = pl.BlockSpec(memory_space=pltpu.VMEM)
    return pl.pallas_call(
        join_kernel,
        in_specs=[pl.BlockSpec(memory_space=pltpu.SMEM)] + [vmem] * 10,
        out_specs=vmem,
        out_shape=jax.ShapeDtypeStruct((q.shape[0], w.shape[1]), jnp.bfloat16),
        cost_estimate=pl.CostEstimate(
            flops=10_000_000_000, bytes_accessed=8_000_000, transcendentals=100_000
        ),
        name="join_part",
    )(index, ps, q, y, r, k, v, gate, tw, hg, w)


def weights_kernel(inner, outer, g_ref, u_ref, d_ref, g_out, u_out, d_out, s1, r1, s2, r2, own_sem):
    me = lax.axis_index("sp")
    a, b = me // outer, me % outer
    wide = g_out.shape[2]

    def peer_a(step):
        return (a + step + inner) % inner * outer + b

    def peer_b(step):
        return a * outer + (b + step + outer) % outer

    barrier = pltpu.get_barrier_semaphore()
    for step in range(1, inner):
        pl.semaphore_signal(barrier, inc=1, device_id={"sp": peer_a(step)}, device_id_type=MESH)
    for step in range(1, outer):
        pl.semaphore_signal(barrier, inc=1, device_id={"sp": peer_b(step)}, device_id_type=MESH)
    pl.semaphore_wait(barrier, inner - 1 + outer - 1)
    outs = (g_out, u_out, d_out)

    def cut(which, part):
        at = pl.ds(pl.multiple_of(part * wide, 128), wide)
        return d_ref.at[at, :] if which == 2 else (g_ref, u_ref)[which].at[:, at]

    def send(src, dst, send_sem, recv_sem, target):
        copy = pltpu.make_async_remote_copy(
            src_ref=src,
            dst_ref=dst,
            send_sem=send_sem,
            recv_sem=recv_sem,
            device_id={"sp": target},
            device_id_type=MESH,
        )
        copy.start()
        return copy

    waits, early = [], {}
    for step in range(1, inner):
        for w in range(3):
            early[step, w] = send(
                cut(w, (a + step) % inner), outs[w].at[me], s1.at[step, w], r1.at[step, w], peer_a(step)
            )
    for w in range(3):
        copy = pltpu.make_async_copy(cut(w, a), outs[w].at[me], own_sem.at[w])
        copy.start()
        waits.append(copy)
    for step in range(inner):
        slot = peer_a(-step)
        for w in range(3):
            if step:
                early[step, w].wait()
            src = outs[w].at[slot] if step else cut(w, a)
            for hop in range(1, outer):
                waits.append(
                    send(src, outs[w].at[slot], s2.at[step, hop, w], r2.at[step, hop, w], peer_b(hop))
                )
    for copy in waits:
        copy.wait()


def spread_weights(inner, w_gate, w_up, w_down):
    sp = lax.axis_size("sp")
    outer = sp // inner
    rows, cols = w_gate.shape
    wide = cols // inner
    vmem = pl.BlockSpec(memory_space=pltpu.VMEM)
    wide_shape = jax.ShapeDtypeStruct((sp, rows, wide), w_gate.dtype)
    tall_shape = jax.ShapeDtypeStruct((sp, wide, w_down.shape[1]), w_down.dtype)
    sems = pltpu.SemaphoreType.DMA
    return pl.pallas_call(
        functools.partial(weights_kernel, inner, outer),
        in_specs=[vmem] * 3,
        out_specs=[vmem] * 3,
        out_shape=[wide_shape, wide_shape, tall_shape],
        scratch_shapes=[
            sems((inner, 3)),
            sems((inner, 3)),
            sems((inner, outer, 3)),
            sems((inner, outer, 3)),
            sems((3,)),
        ],
        compiler_params=pltpu.CompilerParams(
            collective_id=0, has_side_effects=True, vmem_limit_bytes=40 * 1024 * 1024
        ),
        cost_estimate=pl.CostEstimate(
            flops=50_000_000_000, bytes_accessed=100_000_000, transcendentals=0
        ),
        name="spread_weights",
    )(w_gate, w_up, w_down)


def rms_scale(rows, gain):
    x = rows.astype(jnp.float32)
    factor = lax.rsqrt(jnp.mean(x * x, axis=-1, keepdims=True) + NORM_EPS)
    return (x * factor * gain[None]).astype(jnp.bfloat16)


def per_device(r, k, v, dw, lw, gate, tw, hg, w_out, residual, gain, w_gate, w_up, w_down):
    steps = r.shape[0]
    sp, tp = lax.axis_size("sp"), lax.axis_size("tp")
    fits = sp % INNER == 0 and w_gate.shape[1] % (INNER * LANES) == 0
    inner = INNER if fits else 1
    outer = sp // inner
    near = [[i * outer + j for i in range(inner)] for j in range(outer)]
    hidden = w_gate.shape[1] // inner

    q, y, ps = recurrence(r, k, v, dw, lw)
    ps_all = lax.all_gather(ps, "sp")

    w_gate, w_up, w_down, q = lax.optimization_barrier((w_gate, w_up, w_down, q))
    g_all, u_all, d_all = spread_weights(inner, w_gate, w_up, w_down)
    g_all = g_all.reshape(-1, hidden)
    u_all = u_all.reshape(-1, hidden)
    d_all = jnp.moveaxis(d_all, 0, 1).reshape(hidden, -1)

    index = lax.axis_index("sp").astype(jnp.int32).reshape(1)
    part = join(
        index, ps_all, q, y, r, k, v, gate, tw.reshape(1, -1), hg.reshape(1, -1), w_out
    )
    own_rows = steps // tp
    start = lax.axis_index("tp") * own_rows
    mix = lax.all_to_all(part.reshape(tp, own_rows, -1), "tp", 0, 0)
    mix = jnp.sum(mix.astype(jnp.float32), axis=0).astype(jnp.bfloat16).astype(jnp.float32)
    mine = lax.dynamic_slice_in_dim(residual, start, own_rows, 0)
    after = (mine.astype(jnp.float32) + mix).astype(jnp.bfloat16)
    normed = lax.all_gather(rms_scale(after, gain), "tp", axis=0, tiled=True)
    normed = lax.all_gather(normed, "sp", axis_index_groups=near, axis=0, tiled=True)
    g = jnp.dot(normed, g_all, preferred_element_type=jnp.float32)
    u = jnp.dot(normed, u_all, preferred_element_type=jnp.float32)
    h = (jax.nn.silu(g) * u).astype(jnp.bfloat16)
    down = jnp.dot(h, d_all, preferred_element_type=jnp.float32).astype(jnp.bfloat16)
    down = down.reshape(inner, tp, own_rows, -1)
    down = lax.all_to_all(down, "sp", 0, 0, axis_index_groups=near)
    down = jnp.sum(down.astype(jnp.float32), axis=0).astype(jnp.bfloat16)
    down = lax.all_to_all(down, "tp", 0, 0)
    down = jnp.sum(down.astype(jnp.float32), axis=0)
    return (after.astype(jnp.float32) + down).astype(jnp.bfloat16)


def solution(mesh):
    split_both = P("sp", "tp")
    placed = (split_both,) * 6 + (
        P("tp", None),
        P("tp"),
        P("tp", None),
        P("sp", None),
        P(),
        split_both,
        split_both,
        P("tp", "sp"),
    )
    return jax.shard_map(
        per_device, mesh=mesh, in_specs=placed, out_specs=P(("sp", "tp"), None), check_vma=False
    )
```

```python
import functools

import jax
import jax.numpy as jnp
from jax import lax
from jax.experimental import pallas as pl
from jax.experimental.pallas import tpu as pltpu
from jax.sharding import PartitionSpec as P

HEAD = 64
LANES = 2 * HEAD
GROUP_EPS = 0.00064
NORM_EPS = 1e-06
NN = (((1,), (0,)), ((), ()))
NT = (((1,), (1,)), ((), ()))
TN = (((0,), (0,)), ((), ()))
INNER = 4
MESH = pl.DeviceIdType.MESH


def split(x):
    high = x.astype(jnp.bfloat16)
    return high, (x - high.astype(jnp.float32)).astype(jnp.bfloat16)


def dot1(a, b, dims=NN):
    return lax.dot_general(
        a.astype(jnp.bfloat16), b.astype(jnp.bfloat16), dims, preferred_element_type=jnp.float32
    )


def dot3(a, b, dims=NN):
    ah, al = a if isinstance(a, tuple) else split(a)
    bh, bl = b if isinstance(b, tuple) else split(b)
    d = functools.partial(
        lax.dot_general, dimension_numbers=dims, preferred_element_type=jnp.float32
    )
    return d(ah, bh) + (d(ah, bl) + d(al, bh))


def per_head_sum(x, first):
    s0 = jnp.sum(jnp.where(first, x, 0.0), axis=-1, keepdims=True)
    s1 = jnp.sum(jnp.where(first, 0.0, x), axis=-1, keepdims=True)
    return jnp.where(first, s0, s1)


def block_diag_mask():
    row = lax.broadcasted_iota(jnp.int32, (LANES, LANES), 0)
    col = lax.broadcasted_iota(jnp.int32, (LANES, LANES), 1)
    return row // HEAD == col // HEAD, row == col


def fold(full):
    mask, _ = block_diag_mask()
    kept = jnp.where(mask, full, 0.0)
    return kept[:HEAD] + kept[HEAD:]


def unfold(packed):
    mask, _ = block_diag_mask()
    return jnp.where(mask, jnp.concatenate([packed, packed], axis=0), 0.0)


def local_kernel(r_ref, k_ref, v_ref, dw_ref, lw_ref, q_ref, y_ref, ps_ref):
    steps = r_ref.shape[0]
    f32 = jnp.float32
    first = lax.broadcasted_iota(jnp.int32, (steps, LANES), 1) < HEAD
    row = lax.broadcasted_iota(jnp.int32, (steps, steps), 0)
    col = lax.broadcasted_iota(jnp.int32, (steps, steps), 1)
    r, k, v = (x[...].astype(f32) for x in (r_ref, k_ref, v_ref))
    log_decay = jax.nn.sigmoid(dw_ref[...]) * (-0.6065306597126334)
    ones = (row >= col).astype(jnp.bfloat16)
    h0 = log_decay.astype(jnp.bfloat16)
    rest = log_decay - h0.astype(f32)
    h1 = rest.astype(jnp.bfloat16)
    h2 = (rest - h1.astype(f32)).astype(jnp.bfloat16)
    total = dot1(ones, h0) + (dot1(ones, h1) + dot1(ones, h2))
    last = total[steps - 1 :, :]
    unit = k / jnp.maximum(jnp.sqrt(per_head_sum(k * k, first)), 1.0)
    insert = unit * jax.nn.sigmoid(lw_ref[...])
    undo = jnp.exp(-total)
    remaining = jnp.exp(last - total)
    a_bar = -unit * jnp.exp(total - log_decay)
    r_bar = r * jnp.exp(total)
    b_hat = insert * undo
    k_hat = k * undo
    right = split(jnp.concatenate([b_hat, k_hat], axis=0))
    left = jnp.concatenate([a_bar, r_bar], axis=0)
    first2 = jnp.concatenate([first, first], axis=0)
    grams = [
        dot3(jnp.where(first2 if h == 0 else ~first2, left, 0.0), right, NT) for h in (0, 1)
    ]
    strict, incl = row > col, row >= col
    ab = [jnp.where(strict, g[:steps, :steps], 0.0) for g in grams]
    ak = [jnp.where(strict, g[:steps, steps:], 0.0) for g in grams]
    rb = [jnp.where(incl, g[steps:, :steps], 0.0) for g in grams]
    rk = [jnp.where(incl, g[steps:, steps:], 0.0) for g in grams]
    vb = v_ref[...]

    def times_v(m):
        mh, ml = split(m)
        return dot1(mh, vb) + dot1(ml, vb)

    seeds = [jnp.concatenate([a_bar, times_v(m)], axis=1) for m in ak]
    ab16 = [m.astype(jnp.bfloat16) for m in ab]
    eye = (row == col).astype(f32)
    size = 1
    inv = None
    while size < steps:
        joined = (
            (row // (2 * size) == col // (2 * size))
            & ((row // size) % 2 == 1)
            & ((col // size) % 2 == 0)
        )
        parts = [jnp.where(joined, m, jnp.zeros_like(m)) for m in ab16]
        if inv is None:
            inv = [eye + p.astype(f32) for p in parts]
        else:
            t16 = [t.astype(jnp.bfloat16) for t in inv]
            mid = [dot1(t, p) for t, p in zip(t16, parts)]
            inv = [t + dot1(m, tt) for t, m, tt in zip(inv, mid, t16)]
        size *= 2
    inv16 = [t.astype(jnp.bfloat16) for t in inv]
    absp = [split(m) for m in ab]
    sol = [dot1(t, s) for t, s in zip(inv16, seeds)]
    for _ in range(2):
        res = [s - x + dot3(m, x) for s, x, m in zip(seeds, sol, absp)]
        sol = [x + dot1(t, e) for x, t, e in zip(sol, inv16, res)]
    outs = [dot3(m, x) for m, x in zip(rb, sol)]
    own = [times_v(m) for m in rk]
    q_ref[...] = r_bar + jnp.where(first, outs[0][:, :LANES], outs[1][:, :LANES])
    y_ref[...] = jnp.where(first, outs[0][:, LANES:] + own[0], outs[1][:, LANES:] + own[1])
    w = jnp.where(first, sol[0][:, :LANES], sol[1][:, :LANES])
    u = jnp.where(first, sol[0][:, LANES:], sol[1][:, LANES:])
    b_end = split(insert * remaining)
    _, diag = block_diag_mask()
    prod = dot3(w, b_end, TN) + jnp.where(diag, jnp.exp(last), 0.0)
    kh, kl = split(k * remaining)
    state = dot3(u, b_end, TN) + dot1(vb, kh, TN) + dot1(vb, kl, TN)
    ps_ref[0, 0] = fold(prod)
    ps_ref[0, 1] = fold(state)


def join_kernel(i_ref, ps_ref, q_ref, y_ref, r_ref, k_ref, v_ref, g_ref, tw_ref, hg_ref, w_ref, o_ref):
    steps = q_ref.shape[0]
    pairs = q_ref.shape[1] // LANES
    f32 = jnp.float32
    first = lax.broadcasted_iota(jnp.int32, (steps, LANES), 1) < HEAD

    def turn(j, states):
        return tuple(
            dot3(s, unfold(ps_ref[j, p, 0])) + unfold(ps_ref[j, p, 1])
            for p, s in enumerate(states)
        )

    zero = jnp.zeros((LANES, LANES), f32)
    states = lax.fori_loop(0, i_ref[0], turn, (zero,) * pairs)
    mixed = []
    for p in range(pairs):
        cut = slice(p * LANES, (p + 1) * LANES)
        y = dot3(q_ref[:, cut], states[p], NT) + y_ref[:, cut]
        y = y - per_head_sum(y, first) * (1.0 / HEAD)
        spread = per_head_sum(y * y, first) * (1.0 / HEAD)
        r, k, v = (x[:, cut].astype(f32) for x in (r_ref, k_ref, v_ref))
        own = per_head_sum(r * k * tw_ref[:, cut], first) * v
        out = y * lax.rsqrt(spread + GROUP_EPS) * hg_ref[:, cut] + own
        mixed.append((out * jax.nn.sigmoid(g_ref[:, cut].astype(f32))).astype(jnp.bfloat16))
    mixed = jnp.concatenate(mixed, axis=1)
    o_ref[...] = jnp.dot(mixed, w_ref[...], preferred_element_type=f32).astype(jnp.bfloat16)


def recurrence(r, k, v, dw, lw):
    steps, width = r.shape
    pairs = width // LANES
    cols = pl.BlockSpec((steps, LANES), lambda p: (0, p))
    return pl.pallas_call(
        local_kernel,
        grid=(pairs,),
        in_specs=[cols] * 5,
        out_specs=[cols, cols, pl.BlockSpec((1, 2, HEAD, LANES), lambda p: (p, 0, 0, 0))],
        out_shape=[
            jax.ShapeDtypeStruct((steps, width), jnp.float32),
            jax.ShapeDtypeStruct((steps, width), jnp.float32),
            jax.ShapeDtypeStruct((pairs, 2, HEAD, LANES), jnp.float32),
        ],
        cost_estimate=pl.CostEstimate(
            flops=20_000_000_000, bytes_accessed=4_000_000, transcendentals=1_000_000
        ),
        name="local_part",
    )(r, k, v, dw, lw)


def join(index, ps, q, y, r, k, v, gate, tw, hg, w):
    vmem = pl.BlockSpec(memory_space=pltpu.VMEM)
    return pl.pallas_call(
        join_kernel,
        in_specs=[pl.BlockSpec(memory_space=pltpu.SMEM)] + [vmem] * 10,
        out_specs=vmem,
        out_shape=jax.ShapeDtypeStruct((q.shape[0], w.shape[1]), jnp.bfloat16),
        cost_estimate=pl.CostEstimate(
            flops=10_000_000_000, bytes_accessed=8_000_000, transcendentals=100_000
        ),
        name="join_part",
    )(index, ps, q, y, r, k, v, gate, tw, hg, w)


def weights_kernel(inner, outer, g_ref, u_ref, d_ref, g_out, u_out, d_out, s1, r1, s2, r2, own_sem):
    me = lax.axis_index("sp")
    a, b = me // outer, me % outer
    wide = g_out.shape[2]

    def peer_a(step):
        return (a + step + inner) % inner * outer + b

    def peer_b(step):
        return a * outer + (b + step + outer) % outer

    barrier = pltpu.get_barrier_semaphore()
    for step in range(1, inner):
        pl.semaphore_signal(barrier, inc=1, device_id={"sp": peer_a(step)}, device_id_type=MESH)
    for step in range(1, outer):
        pl.semaphore_signal(barrier, inc=1, device_id={"sp": peer_b(step)}, device_id_type=MESH)
    pl.semaphore_wait(barrier, inner - 1 + outer - 1)
    outs = (g_out, u_out, d_out)

    def cut(which, part):
        at = pl.ds(pl.multiple_of(part * wide, 128), wide)
        return d_ref.at[at, :] if which == 2 else (g_ref, u_ref)[which].at[:, at]

    def send(src, dst, send_sem, recv_sem, target):
        copy = pltpu.make_async_remote_copy(
            src_ref=src,
            dst_ref=dst,
            send_sem=send_sem,
            recv_sem=recv_sem,
            device_id={"sp": target},
            device_id_type=MESH,
        )
        copy.start()
        return copy

    waits, early = [], {}
    for step in range(1, inner):
        for w in range(3):
            early[step, w] = send(
                cut(w, (a + step) % inner), outs[w].at[me], s1.at[step, w], r1.at[step, w], peer_a(step)
            )
    for w in range(3):
        copy = pltpu.make_async_copy(cut(w, a), outs[w].at[me], own_sem.at[w])
        copy.start()
        waits.append(copy)
    for step in range(inner):
        slot = peer_a(-step)
        for w in range(3):
            if step:
                early[step, w].wait()
            src = outs[w].at[slot] if step else cut(w, a)
            for hop in range(1, outer):
                waits.append(
                    send(src, outs[w].at[slot], s2.at[step, hop, w], r2.at[step, hop, w], peer_b(hop))
                )
    for copy in waits:
        copy.wait()


def spread_weights(inner, w_gate, w_up, w_down):
    sp = lax.axis_size("sp")
    outer = sp // inner
    rows, cols = w_gate.shape
    wide = cols // inner
    vmem = pl.BlockSpec(memory_space=pltpu.VMEM)
    wide_shape = jax.ShapeDtypeStruct((sp, rows, wide), w_gate.dtype)
    tall_shape = jax.ShapeDtypeStruct((sp, wide, w_down.shape[1]), w_down.dtype)
    sems = pltpu.SemaphoreType.DMA
    return pl.pallas_call(
        functools.partial(weights_kernel, inner, outer),
        in_specs=[vmem] * 3,
        out_specs=[vmem] * 3,
        out_shape=[wide_shape, wide_shape, tall_shape],
        scratch_shapes=[
            sems((inner, 3)),
            sems((inner, 3)),
            sems((inner, outer, 3)),
            sems((inner, outer, 3)),
            sems((3,)),
        ],
        compiler_params=pltpu.CompilerParams(
            collective_id=0, has_side_effects=True, vmem_limit_bytes=40 * 1024 * 1024
        ),
        cost_estimate=pl.CostEstimate(
            flops=50_000_000_000, bytes_accessed=100_000_000, transcendentals=0
        ),
        name="spread_weights",
    )(w_gate, w_up, w_down)


def rows_kernel(inner, tp, scatter, x_ref, out_ref, s1, r1, s2, r2, own_sem):
    sp_at, t = lax.axis_index("sp"), lax.axis_index("tp")
    outer = lax.axis_size("sp") // inner
    a, b = sp_at // outer, sp_at % outer
    barrier = pltpu.get_barrier_semaphore()

    def at(step):
        return (a + step + inner) % inner

    def far(step):
        return {"sp": at(step) * outer + b, "tp": t}

    def near(step):
        return {"sp": sp_at, "tp": (t + step) % tp}

    near_steps = () if scatter else range(1, tp)
    for step in range(1, inner):
        pl.semaphore_signal(barrier, inc=1, device_id=far(step), device_id_type=MESH)
    for step in near_steps:
        pl.semaphore_signal(barrier, inc=1, device_id=near(step), device_id_type=MESH)
    pl.semaphore_wait(barrier, inner - 1 + len(near_steps))

    def send(src, dst, send_sem, recv_sem, target):
        copy = pltpu.make_async_remote_copy(
            src_ref=src,
            dst_ref=dst,
            send_sem=send_sem,
            recv_sem=recv_sem,
            device_id=target,
            device_id_type=MESH,
        )
        copy.start()
        return copy

    def slot(which):
        return out_ref.at[which] if scatter else out_ref.at[t, which]

    early = {}
    for step in range(1, inner):
        src = x_ref.at[at(step)] if scatter else x_ref
        early[step] = send(src, slot(a), s1.at[step], r1.at[step], far(step))
    own = pltpu.make_async_copy(x_ref.at[a] if scatter else x_ref, slot(a), own_sem)
    own.start()
    waits = [own]
    for step in range(inner):
        if step:
            early[step].wait()
        for hop in near_steps:
            src = slot(at(-step)) if step else x_ref
            waits.append(
                send(src, slot(at(-step)), s2.at[step, hop], r2.at[step, hop], near(hop))
            )
    for copy in waits:
        copy.wait()


def move_rows(x, inner, scatter):
    tp = lax.axis_size("tp")
    shape = x.shape if scatter else (tp, inner) + x.shape
    sems = pltpu.SemaphoreType.DMA
    vmem = pl.BlockSpec(memory_space=pltpu.VMEM)
    return pl.pallas_call(
        functools.partial(rows_kernel, inner, tp, scatter),
        in_specs=[vmem],
        out_specs=vmem,
        out_shape=jax.ShapeDtypeStruct(shape, x.dtype),
        scratch_shapes=[
            sems((inner,)),
            sems((inner,)),
            sems((inner, tp)),
            sems((inner, tp)),
            sems(()),
        ],
        compiler_params=pltpu.CompilerParams(
            collective_id=1 if scatter else 2, has_side_effects=True
        ),
        cost_estimate=pl.CostEstimate(
            flops=20_000_000_000, bytes_accessed=10_000_000, transcendentals=0
        ),
        name="scatter_rows" if scatter else "gather_rows",
    )(x)


def rms_scale(rows, gain):
    x = rows.astype(jnp.float32)
    factor = lax.rsqrt(jnp.mean(x * x, axis=-1, keepdims=True) + NORM_EPS)
    return (x * factor * gain[None]).astype(jnp.bfloat16)


def per_device(r, k, v, dw, lw, gate, tw, hg, w_out, residual, gain, w_gate, w_up, w_down):
    steps = r.shape[0]
    sp, tp = lax.axis_size("sp"), lax.axis_size("tp")
    fits = sp % INNER == 0 and w_gate.shape[1] % (INNER * LANES) == 0
    inner = INNER if fits else 1
    hidden = w_gate.shape[1] // inner

    q, y, ps = recurrence(r, k, v, dw, lw)
    ps_all = lax.all_gather(ps, "sp")

    w_gate, w_up, w_down, q = lax.optimization_barrier((w_gate, w_up, w_down, q))
    g_all, u_all, d_all = spread_weights(inner, w_gate, w_up, w_down)
    y, g_all, u_all, d_all = lax.optimization_barrier((y, g_all, u_all, d_all))
    g_all = g_all.reshape(-1, hidden)
    u_all = u_all.reshape(-1, hidden)
    d_all = jnp.moveaxis(d_all, 0, 1).reshape(hidden, -1)

    index = lax.axis_index("sp").astype(jnp.int32).reshape(1)
    part = join(
        index, ps_all, q, y, r, k, v, gate, tw.reshape(1, -1), hg.reshape(1, -1), w_out
    )
    own_rows = steps // tp
    start = lax.axis_index("tp") * own_rows
    mix = lax.all_to_all(part.reshape(tp, own_rows, -1), "tp", 0, 0)
    mix = jnp.sum(mix.astype(jnp.float32), axis=0).astype(jnp.bfloat16).astype(jnp.float32)
    mine = lax.dynamic_slice_in_dim(residual, start, own_rows, 0)
    after = (mine.astype(jnp.float32) + mix).astype(jnp.bfloat16)
    normed = move_rows(rms_scale(after, gain), inner, False)
    normed = normed.reshape(tp * inner * own_rows, -1)
    g = jnp.dot(normed, g_all, preferred_element_type=jnp.float32)
    u = jnp.dot(normed, u_all, preferred_element_type=jnp.float32)
    h = (jax.nn.silu(g) * u).astype(jnp.bfloat16)
    down = jnp.dot(h, d_all, preferred_element_type=jnp.float32).astype(jnp.bfloat16)
    down = lax.all_to_all(down.reshape(tp, inner, own_rows, -1), "tp", 0, 0)
    down = jnp.sum(down.astype(jnp.float32), axis=0)
    if inner > 1:
        down = move_rows(down.astype(jnp.bfloat16), inner, True).astype(jnp.float32)
    down = jnp.sum(down, axis=0)
    return (after.astype(jnp.float32) + down).astype(jnp.bfloat16)


def solution(mesh):
    split_both = P("sp", "tp")
    placed = (split_both,) * 6 + (
        P("tp", None),
        P("tp"),
        P("tp", None),
        P("sp", None),
        P(),
        split_both,
        split_both,
        P("tp", "sp"),
    )
    return jax.shard_map(
        per_device, mesh=mesh, in_specs=placed, out_specs=P(("sp", "tp"), None), check_vma=False
    )
```
